512 devices in a mesh: grp: 2 (over y), ep: 16 (over z), tp: 16 (over x, core).
Axes of the slice: x: 8, y: 2, z: 16, core: 2. Of those that a mesh axis runs over, the one named last changes fastest.
The devices are a block of a 8x16x16 slice.
Arguments:
- queries: bfloat16 [8192, 2048], P(('grp', 'ep'), 'tp'), parts along dimension 0, may hold values from -8 to 8
- keys: bfloat16 [8192, 512], P(('grp', 'ep')), parts along dimension 0, may hold values from -8 to 8
- values: bfloat16 [8192, 512], P(('grp', 'ep')), parts along dimension 0, may hold values from -6 to 6
- q_gain: float32 [128], replicated, may hold values from 0.6 to 5.8
- k_gain: float32 [128], replicated, may hold values from 0.6 to 5.8
- w_out: bfloat16 [2048, 2048], P(None, 'tp'), may hold values from -0.125 to 0.125
- moe_rows: bfloat16 [6144, 2048], P(('grp', 'ep')), parts along dimension 0, may hold values from -6 to 6
- routes: int32 [6144, 2], P(('grp', 'ep')), parts along dimension 0, may hold values from 0 to 15, all different within a row; in each aligned block of 192 rows (0 to 191, 192 to 383, ...) at most 36 rows name the same one
- group_gate: float32 [6144], P(('grp', 'ep')), parts along dimension 0, may hold values from 0.25 to 1
- expert_logits: float32 [6144, 2], P(('grp', 'ep')), parts along dimension 0, may hold values from -6 to 6
- moe_gain: float32 [2048], replicated, may hold values from 0.1 to 1.9
- w_gate: bfloat16 [16, 2048, 2048], P('ep', None, 'tp'), may hold values from -0.125 to 0.125
- w_up: bfloat16 [16, 2048, 2048], P('ep', None, 'tp'), may hold values from -0.125 to 0.125
- w_down: bfloat16 [16, 2048, 2048], P('ep', 'tp'), may hold values from -0.125 to 0.125
Outputs:
- attn_out: bfloat16 [8192, 2048], P(('grp', 'ep'), 'tp'), parts along dimension 0
- moe_out: bfloat16 [6144, 2048], P(('grp', 'ep'), 'tp'), parts along dimension 0
The draws below stay inside these ranges and needn't reach their ends.
There are 2 independent parts, one for each index of `grp`. The reference program is written for one: setup_inputs(seed, part) draws one part's arguments, and reference() takes and returns one part's arrays. A program takes and returns all parts, laid end to end along the dimension named above; an argument that names none is the same for every part. Nothing has to cross between parts.
Inputs may be any that keep to these rules, and one draw needn't show every extreme that they name: `routes`: each row names 2 different experts; within the rows of one index of ep no expert is named more than 36 times, a bound that some block reaches.
All inputs are finite; a program needn't handle non-finite values.
Results may differ from the reference program's by a relative error of at most 0.019.
The reference program's roundings to bfloat16 on the way count: a program that leaves them out, or rounds other values in their place, can miss the bound.
Values may be sent and summed in bfloat16 or wider, within the bound.
A program may use at most 64 MiB of HBM per device.

```python
import math
import jax
import jax.numpy as jnp
import numpy as np
from jax import lax

D = 2048
HEADS = 16
KV_HEADS = 4
HEAD_DIM = 128
GRID_W = 64
FF = 2048
TOPK = 2
MOE_DEV = 192
ATT_TOK = 4096
MOE_TOK = 3072
EXPERTS = 16
CAP = 36
N_EP = 16
N_TP = 16


def drawn_keys(key):
    base = jax.random.normal(jax.random.fold_in(key, 7), (ATT_TOK, KV_HEADS * HEAD_DIM), jnp.float32)
    return jnp.clip(base, -8.0, 8.0)


def draw_keys(key, part):
    return drawn_keys(key).astype(jnp.bfloat16)


def draw_queries(key, part):
    own = jax.random.normal(jax.random.fold_in(key, 9), (ATT_TOK, HEADS * HEAD_DIM), jnp.float32)
    return jnp.clip(own, -8.0, 8.0).astype(jnp.bfloat16)


def draw_q_gain(key, part):
    return jax.random.uniform(jax.random.fold_in(key, 11), (HEAD_DIM,), jnp.float32, 0.6, 1.4)


def draw_k_gain(key, part):
    return jax.random.uniform(jax.random.fold_in(key, 13), (HEAD_DIM,), jnp.float32, 0.6, 1.4)


def block_levels(key, extent, cuts, least, high):
    level, own = 1.0, jax.random.fold_in(key, 6)
    for axis_at, shards_of in cuts:
        draws = jnp.exp(jax.random.uniform(jax.random.fold_in(own, axis_at), (shards_of,), jnp.float32, least / len(cuts), high / len(cuts)))
        level = level * jnp.repeat(draws, extent[axis_at] // shards_of).reshape([-1 if axis == axis_at else 1 for axis in range(len(extent))])
    return level


def shared_out(key, own, number, rows, number_of, top, most, skew):
    sequence = jax.random.permutation(key, number_of)
    heavy_load, usual = load_shares(number_of, rows * top, most, skew, True), load_shares(number_of, rows * top, most, skew, False)
    places = jnp.arange(number_of)

    def named(lengths, offset_by):
        used = int((lengths > 0).sum())
        fixed = max(1, used // 4)
        passed = fixed + (places - fixed + offset_by * (used - fixed)) % max(1, number_of - fixed)
        return jnp.zeros((number_of,), jnp.int32).at[sequence[jnp.where(places < fixed, places, passed)]].set(jnp.asarray(lengths, jnp.int32))

    lengths = jnp.where(number % 4 == 0, named(heavy_load, number // 4), named(usual, number - number // 4 - 1))
    mixed = jax.random.permutation(jax.random.fold_in(own, 3), number_of)
    giver, sink = mixed[0:number_of // 2 * 2:2], mixed[1:number_of // 2 * 2:2]
    slack = jnp.minimum(lengths[giver] - 1, most - lengths[sink]) // 2
    slack = jnp.where((giver == sequence[0]) | (sink == sequence[0]) | (lengths[sink] == 0), 0, jnp.maximum(slack, 0))
    passed = jax.random.randint(jax.random.fold_in(own, 4), (number_of // 2,), 0, 1 << 20) % (slack + 1)
    lengths = lengths.at[giver].add(-passed).at[sink].add(passed)
    members = jnp.searchsorted(jnp.cumsum(lengths), jnp.arange(rows * top), side="right").astype(jnp.int32)
    table = members.reshape(top, rows).T
    table = table[jax.random.permutation(jax.random.fold_in(own, 1), rows)]
    offset_by = jax.random.randint(jax.random.fold_in(own, 2), (rows, 1), 0, top)
    return jnp.take_along_axis(table, (jnp.arange(top)[None, :] + offset_by) % top, axis=1)


def load_shares(number_of, total, most, slope, full):
    weights = [(1 << 20) // math.isqrt(grade ** slope) + 1 for grade in range(1, number_of + 1)]
    largest = most if full else min(most, max(-(-total // number_of), total * weights[0] // sum(weights)))
    least = 1 if total - largest >= number_of - 1 else 0
    counts, rest = [largest] + [least] * (number_of - 1), total - largest - least * (number_of - 1)
    while rest > 0:
        free = [i for i in range(1, number_of) if counts[i] < largest] or [i for i in range(1, number_of) if counts[i] < most]
        mass, remaining = sum([weights[i] for i in free]), rest
        for i in free:
            addition = min(most - counts[i], max(1, remaining * weights[i] // mass), rest)
            counts[i] = counts[i] + addition
            rest = rest - addition
    return np.array(counts)


def bell_draw(rng, extent, deviation, reach, cuts=(), held_as=jnp.bfloat16):
    values = deviation * jax.random.normal(rng, extent, jnp.float32)
    if cuts:
        values = values * block_levels(rng, extent, cuts, -0.22, 0.18)
    return jnp.clip(values, -reach, reach).astype(held_as)


def setup_inputs(seed: int = 0, part: int = 0) -> dict:
    key_list = jax.random.split(jax.random.key(seed), 15)
    part_keys = jax.random.split(jax.random.fold_in(key_list[14], part), 15)
    queries = draw_queries(jax.random.fold_in(jax.random.fold_in(key_list[14], part), 71), part)
    keys = draw_keys(jax.random.fold_in(jax.random.fold_in(key_list[14], part), 71), part)
    values = bell_draw(part_keys[2], (ATT_TOK, KV_HEADS * HEAD_DIM), 1.0, 6.0, ((0, 16),))
    q_gain = draw_q_gain(jax.random.fold_in(key_list[14], 71), part)
    k_gain = draw_k_gain(jax.random.fold_in(key_list[14], 71), part)
    w_out = bell_draw(key_list[5], (HEADS * HEAD_DIM, D), (HEADS * HEAD_DIM) ** -0.5, 0.125, ((1, 16),))
    moe_rows = bell_draw(part_keys[6], (MOE_TOK, D), 1.0, 6.0, ((0, 16),))
    routes_keys = jax.random.split(jax.random.fold_in(part_keys[7], 1), MOE_TOK // MOE_DEV)
    routes_turns = jax.random.permutation(jax.random.fold_in(part_keys[7], 3), MOE_TOK // MOE_DEV)
    routes = jax.vmap(lambda own, number: shared_out(jax.random.fold_in(part_keys[7], 2), own, number, MOE_DEV, EXPERTS, TOPK, CAP, 1))(routes_keys, routes_turns).reshape((MOE_TOK, TOPK))
    group_gate = jnp.clip(jnp.exp(math.log(1.0) - 1.3862944 * jax.random.uniform(part_keys[8], (MOE_TOK,), jnp.float32) ** block_levels(part_keys[8], (MOE_TOK,), ((0, 16),), -0.2, 0.2)), 0.25, 1.0)
    expert_logits = bell_draw(part_keys[9], (MOE_TOK, TOPK), 1.5, 6.0, ((0, 16),), jnp.float32)
    moe_gain = jnp.clip(1.0 + 0.18 * jax.random.normal(key_list[10], (D,), jnp.float32), 0.1, 1.9)
    w_gate = bell_draw(key_list[11], (EXPERTS, D, FF), D ** -0.5, 0.125, ((0, 16), (2, 16)))
    w_up = bell_draw(key_list[12], (EXPERTS, D, FF), D ** -0.5, 0.125, ((0, 16), (2, 16)))
    w_down = bell_draw(key_list[13], (EXPERTS, FF, D), FF ** -0.5, 0.125, ((0, 16), (1, 16)))
    return {"queries": queries, "keys": keys, "values": values, "q_gain": q_gain, "k_gain": k_gain, "w_out": w_out, "moe_rows": moe_rows, "routes": routes, "group_gate": group_gate, "expert_logits": expert_logits, "moe_gain": moe_gain, "w_gate": w_gate, "w_up": w_up, "w_down": w_down}


def rope_tables(count):
    pos = jnp.arange(count, dtype=jnp.int32)
    row = (pos // GRID_W).astype(jnp.float32)
    col = (pos % GRID_W).astype(jnp.float32)
    nfreq = HEAD_DIM // 4
    inverse = 10000.0 ** (-jnp.arange(nfreq, dtype=jnp.float32) / nfreq)
    angle = jnp.concatenate([row[:, None] * inverse, row[:, None] * inverse, col[:, None] * inverse, col[:, None] * inverse], axis=1)
    return (jnp.cos(angle), jnp.sin(angle))

def rotate(x, cosine, sine):
    parts = x.reshape(x.shape[:-1] + (2, 2, HEAD_DIM // 4))
    turned = jnp.stack([-parts[..., 1, :], parts[..., 0, :]], axis=-2).reshape(x.shape)
    return x * cosine[:, None, :] + turned * sine[:, None, :]

def head_norm(x, gain):
    wide = x.astype(jnp.float32)
    return wide * lax.rsqrt(lax.optimization_barrier(jnp.mean(wide * wide, axis=-1, keepdims=True)) + 1e-06) * gain

def attend(query, key_rows, value_rows):
    scores = jnp.dot(query, key_rows.T, preferred_element_type=jnp.float32) * HEAD_DIM ** (-0.5)
    top = lax.optimization_barrier(jnp.max(scores, axis=-1, keepdims=True))
    expo = jnp.exp(scores - top)
    total = lax.optimization_barrier(jnp.sum(expo, axis=-1, keepdims=True))
    mixed = jnp.dot(expo.astype(jnp.bfloat16), value_rows, preferred_element_type=jnp.float32) / total
    return mixed.astype(jnp.bfloat16)

def slot_table(chosen):
    onehot = (chosen[:, None] == jnp.arange(EXPERTS, dtype=jnp.int32)[None, :]).astype(jnp.int32)
    rank = lax.optimization_barrier(jnp.sum((jnp.cumsum(onehot, axis=0) - onehot) * onehot, axis=1))
    return chosen * CAP + rank

def reference(queries, keys, values, q_gain, k_gain, w_out, moe_rows, routes, group_gate, expert_logits, moe_gain, w_gate, w_up, w_down):
    count = queries.shape[0]
    group = HEADS // KV_HEADS
    cosine, sine = rope_tables(count)
    q_rot = rotate(head_norm(queries.reshape(count, HEADS, HEAD_DIM), q_gain), cosine, sine).astype(jnp.bfloat16)
    k_rot = rotate(head_norm(keys.reshape(count, KV_HEADS, HEAD_DIM), k_gain), cosine, sine).astype(jnp.bfloat16)
    q_heads = q_rot.reshape(count, KV_HEADS, group, HEAD_DIM).transpose(1, 2, 0, 3)
    k_heads = k_rot.transpose(1, 0, 2)
    v_heads = values.reshape(count, KV_HEADS, HEAD_DIM).transpose(1, 0, 2)

    def per_key_head(items):
        q_group, key_rows, value_rows = items
        return lax.map(lambda query: attend(query, key_rows, value_rows), q_group)
    heads_out = lax.map(per_key_head, (q_heads, k_heads, v_heads))
    joined = heads_out.transpose(2, 0, 1, 3).reshape(count, HEADS * HEAD_DIM)
    attn_out = jnp.dot(joined, w_out, preferred_element_type=jnp.float32).astype(jnp.bfloat16)
    width = moe_rows.shape[1]
    wide = moe_rows.astype(jnp.float32)
    normed = (wide * lax.rsqrt(lax.optimization_barrier(jnp.mean(wide * wide, axis=-1, keepdims=True)) + 1e-06) * moe_gain).astype(jnp.bfloat16)
    blocks = normed.reshape(N_EP, MOE_DEV, width)
    chosen = routes.reshape(N_EP, MOE_DEV * TOPK)
    slots = jax.vmap(slot_table)(chosen)
    owner = jnp.arange(MOE_DEV * TOPK, dtype=jnp.int32) // TOPK

    def fill(block, slot):
        source = jnp.zeros((EXPERTS * CAP,), jnp.int32).at[slot].set(owner)
        used = jnp.zeros((EXPERTS * CAP,), jnp.bool_).at[slot].set(True)
        return jnp.where(used[:, None], block[source], jnp.zeros((), jnp.bfloat16))
    buffers = jax.vmap(fill)(blocks, slots)
    per_expert = buffers.reshape(N_EP, EXPERTS, CAP, width).transpose(1, 0, 2, 3).reshape(EXPERTS, N_EP * CAP, width)
    part_ff = FF // N_TP

    def expert(items):
        rows, gate_w, up_w, down_w = items
        gate = jnp.dot(rows, gate_w, preferred_element_type=jnp.float32)
        up = jnp.dot(rows, up_w, preferred_element_type=jnp.float32)
        hidden = (jax.nn.silu(gate) * up).astype(jnp.bfloat16)
        pieces = jnp.einsum('rtf,tfd->rtd', hidden.reshape(-1, N_TP, part_ff).astype(jnp.float32), down_w.reshape(N_TP, part_ff, width).astype(jnp.float32))
        return lax.optimization_barrier(jnp.sum(pieces.astype(jnp.bfloat16).astype(jnp.float32), axis=1)).astype(jnp.bfloat16)
    results = lax.map(expert, (per_expert, w_gate, w_up, w_down))
    by_source = results.reshape(EXPERTS, N_EP, CAP, width).transpose(1, 0, 2, 3).reshape(N_EP, EXPERTS * CAP, width)
    picked = jax.vmap(lambda table, slot: table[slot])(by_source, slots)
    picked = picked.astype(jnp.float32).reshape(N_EP * MOE_DEV, TOPK, width)
    weights = group_gate[:, None] * jax.nn.softmax(expert_logits, axis=-1)
    moe_out = lax.optimization_barrier(jnp.sum(weights[:, :, None] * picked, axis=1)).astype(jnp.bfloat16)
    return (attn_out, moe_out)
```

```python
import functools

import jax
import jax.numpy as jnp
from jax import lax
from jax.experimental import pallas as pl
from jax.experimental.pallas import tpu as pltpu
from jax.sharding import PartitionSpec as P

HEADS = 16
KV_HEADS = 4
HEAD_DIM = 128
GRID_W = 64
TOPK = 2
W = 128
PAD = 48
MESH = pl.DeviceIdType.MESH
f32 = jnp.float32
bf16 = jnp.bfloat16


def remote(src, dst, ss, rs, dev):
    return pltpu.make_async_remote_copy(
        src_ref=src, dst_ref=dst, send_sem=ss, recv_sem=rs, device_id=dev, device_id_type=MESH
    )


def near_first(n):
    order = [0]
    for i in range(1, n // 2 + 1):
        order += [i] if 2 * i == n else [i, n - i]
    return order


def moe_kernel(
    nz,
    nt,
    rows_hbm,
    routes_ref,
    ggate_ref,
    logits_ref,
    gain_ref,
    wg_hbm,
    wu_hbm,
    wd_hbm,
    out_ref,
    rows_v,
    w13,
    wdp,
    sendb,
    recvb,
    xall,
    pairs,
    psend,
    precv,
    rs_send,
    rs_recv,
    ret_send,
    ret_recv,
    smat,
    lsem,
    wsem,
    disp_s,
    disp_r,
    ag_s,
    ag_r,
    dd_s,
    dd_r,
    pr_s,
    pr_r,
    rss_s,
    rss_r,
    ret_s,
    ret_r,
):
    count, width = rows_v.shape
    nx = nt // 2
    half = nx // 2
    cap = 3 * count // nz
    nchunk = nz // 4
    R = 4 * cap
    RP = 4 * PAD
    up_rows = 80
    order = near_first(nz)
    pos = {d: p for p, d in enumerate(order)}
    color = nx * W

    z = lax.axis_index("ep")
    t = lax.axis_index("tp")
    x = t // 2
    c = t % 2
    right = ((x + 1) % nx) * 2 + c
    left = ((x + nx - 1) % nx) * 2 + c
    other = x * 2 + (1 - c)

    def lane(i):
        return pl.ds(pl.multiple_of(i * W, W), W)

    barrier = pltpu.get_barrier_semaphore()
    for d in order[1:][::-1]:
        pl.semaphore_signal(barrier, inc=1, device_id={"ep": (z + d) % nz}, device_id_type=MESH)
    for who in (right, left, other):
        pl.semaphore_signal(barrier, inc=1, device_id={"tp": who}, device_id_type=MESH)

    load_rows = pltpu.make_async_copy(rows_hbm, rows_v, lsem.at[0])
    load_g = pltpu.make_async_copy(wg_hbm, w13.at[:, 0:W], lsem.at[1])
    load_u = pltpu.make_async_copy(wu_hbm, w13.at[:, W : 2 * W], lsem.at[2])
    load_rows.start()
    load_g.start()
    load_u.start()
    load_d = []
    for k in range(2):
        for dx in range(nx):
            core = c if k == 0 else 1 - c
            col = ((x + dx) % nx) * 2 + core
            at = k * color + dx * W
            load_d.append(
                pltpu.make_async_copy(
                    wd_hbm.at[:, lane(col)], wdp.at[:, at : at + W], wsem.at[k * nx + dx]
                )
            )
            load_d[-1].start()

    e_lane = lax.broadcasted_iota(jnp.int32, (count, W), 1)
    r0 = routes_ref[:, 0:1]
    r1 = routes_ref[:, 1:2]
    named = jnp.where((r0 == e_lane) | (r1 == e_lane), 1.0, 0.0).astype(bf16)
    named0 = jnp.where(r0 == e_lane, 1.0, 0.0).astype(bf16)
    before = jnp.where(
        lax.broadcasted_iota(jnp.int32, (count, count), 1)
        < lax.broadcasted_iota(jnp.int32, (count, count), 0),
        1.0,
        0.0,
    ).astype(bf16)
    rank = jnp.dot(before, named, preferred_element_type=f32).astype(bf16)
    col_e = lax.broadcasted_iota(jnp.int32, (W, nz * PAD), 1)
    row_e = lax.broadcasted_iota(jnp.int32, (W, nz * PAD), 0)
    lo = row_e * PAD
    spread = jnp.where((col_e >= lo) & (col_e < lo + PAD), 1.0, 0.0).astype(bf16)
    slot_of = (
        lax.broadcasted_iota(jnp.int32, (1, nz * PAD), 1) % PAD
    ).astype(f32)
    named_x = jnp.dot(named, spread, preferred_element_type=f32)
    named0_x = jnp.dot(named0, spread, preferred_element_type=f32)
    rank_x = jnp.dot(rank, spread, preferred_element_type=f32)
    hit = (named_x > 0.5) & (jnp.abs(rank_x - slot_of) < 0.5)
    hit0 = hit & (named0_x > 0.5)
    s_all = jnp.where(hit, 1.0, 0.0)
    s_0 = jnp.where(hit0, 1.0, 0.0)
    smat[0] = s_0.astype(bf16)
    smat[1] = (s_all - s_0).astype(bf16)

    load_rows.wait()
    wide = rows_v[...].astype(f32)
    inv = lax.rsqrt(jnp.mean(wide * wide, axis=-1, keepdims=True) + 1e-06)
    mine = rows_v[:, lane(t)].astype(f32) * inv * gain_ref[:, lane(t)]
    sendb[...] = lax.dot_general(
        s_all.astype(bf16), mine.astype(bf16), (((0,), (0,)), ((), ())), preferred_element_type=f32
    ).astype(bf16)

    pl.semaphore_wait(barrier, nz - 1 + 3)

    def block(i):
        return pl.ds(pl.multiple_of(i * PAD, PAD), PAD)

    def disp(d):
        to = (z + d) % nz
        p = pos[(nz - d) % nz]
        return remote(
            sendb.at[block(to)],
            recvb.at[p * PAD : (p + 1) * PAD],
            disp_s.at[d],
            disp_r.at[p],
            {"ep": to},
        )

    def disp_in(p):
        d = (nz - order[p]) % nz
        return disp(d)

    for d in order[1:]:
        disp(d).start()
    recvb[0:PAD] = sendb[block(z)]

    pr = lax.broadcasted_iota(jnp.int32, (R, RP), 0)
    pc = lax.broadcasted_iota(jnp.int32, (R, RP), 1)
    pack = jnp.where((pr // cap == pc // PAD) & (pr % cap == pc % PAD), 1.0, 0.0).astype(bf16)

    def at_rows(k):
        return pl.ds(pl.multiple_of(k * R, R), R)

    def ag(k, side, s):
        xo = (x + nx - (s - 1)) % nx if side == 0 else (x + s - 1) % nx
        cols = lane(xo * 2 + c)
        if s < half:
            part = at_rows(k)
        elif side == 0:
            part = pl.ds(pl.multiple_of(k * R, 16), up_rows)
        else:
            part = pl.ds(pl.multiple_of(k * R + up_rows, 16), R - up_rows)
        view = xall.at[part, cols]
        to = right if side == 0 else left
        return remote(view, view, ag_s.at[k, side, s - 1], ag_r.at[k, side, s - 1], {"tp": to})

    def ag_in(k, side, s):
        return ag(k, side, s)

    def dd(k, j, mine_side):
        core = c if mine_side else 1 - c
        rows = at_rows(k)
        if j == 0:
            xo = x
        elif j <= half - 1:
            xo = (x + nx - j) % nx
        elif j <= 2 * half - 2:
            xo = (x + j - (half - 1)) % nx
        else:
            xo = (x + half) % nx
            if j == 2 * half - 1:
                rows = pl.ds(pl.multiple_of(k * R, 16), up_rows)
            else:
                rows = pl.ds(pl.multiple_of(k * R + up_rows, 16), R - up_rows)
        view = xall.at[rows, lane(xo * 2 + core)]
        return remote(view, view, dd_s.at[k, j], dd_r.at[k, j], {"tp": other})

    ndd = 2 * half + 1

    for k in range(nchunk):
        for p in range(4 * k, 4 * k + 4):
            if p:
                disp_in(p).wait_recv()
        packed = jnp.dot(pack, recvb[k * RP : (k + 1) * RP], preferred_element_type=f32)
        xall[k * R : (k + 1) * R, lane(t)] = packed.astype(bf16)
        ag(k, 0, 1).start()
        ag(k, 1, 1).start()
        dd(k, 0, True).start()

    for s in range(1, half + 1):

        def hop(k, carry, s=s):
            for side in range(2):
                ag_in(k, side, s).wait_recv()
                if s < half:
                    ag(k, side, s + 1).start()
                    dd(k, s if side == 0 else half - 1 + s, True).start()
                else:
                    dd(k, 2 * half - 1 + side, True).start()
            return carry

        lax.fori_loop(0, nchunk, hop, 0)

    load_g.wait()
    load_u.wait()
    for cp in load_d:
        cp.wait()

    def pair(k):
        return remote(psend.at[k], precv.at[k], pr_s.at[k], pr_r.at[k], {"tp": other})

    def ffn(k, carry):
        for j in range(ndd):
            dd(k, j, False).wait_recv()
        xk = xall[at_rows(k), :]
        h = jnp.dot(xk, w13[...], preferred_element_type=f32)
        g = h[:, 0:W]
        hidden = (g * jax.nn.sigmoid(g) * h[:, W : 2 * W]).astype(bf16)
        part = jnp.dot(hidden, wdp[...], preferred_element_type=f32).astype(bf16)
        psend[k] = part[:, color:]
        pairs[k] = part[:, :color].astype(f32)
        pair(k).start()
        return carry

    lax.fori_loop(0, nchunk, ffn, 0)

    def part_rows(side, s):
        if s > 1:
            return 0, R
        return (0, up_rows) if side == 0 else (up_rows, R)

    def rs(k, side, s):
        a, b = part_rows(side, s)
        to = right if side == 0 else left
        return remote(
            rs_send.at[k, side, s - 1, a:b],
            rs_recv.at[k, side, s - 1, a:b],
            rss_s.at[k, side, s - 1],
            rss_r.at[k, side, s - 1],
            {"tp": to},
        )

    def target(side, s):
        far = half + 1 - s
        return far if side == 0 else nx - far

    def rs_first(k, carry):
        pair(k).wait_recv()
        pairs[k] = pairs[k] + precv[k].astype(f32)
        for side in range(2):
            a, b = part_rows(side, 1)
            at = target(side, 1) * W
            rs_send[k, side, 0, a:b] = pairs[k, a:b, at : at + W].astype(bf16)
            rs(k, side, 1).start()
        return carry

    lax.fori_loop(0, nchunk, rs_first, 0)

    for s in range(2, half + 1):

        def rs_hop(k, carry, s=s):
            for side in range(2):
                rs(k, side, s - 1).wait_recv()
                at = target(side, s) * W
                a, b = part_rows(side, s - 1)
                rs_send[k, side, s - 1, a:b] = (
                    pairs[k, a:b, at : at + W] + rs_recv[k, side, s - 2, a:b].astype(f32)
                ).astype(bf16)
                if a > 0:
                    rs_send[k, side, s - 1, 0:a] = pairs[k, 0:a, at : at + W].astype(bf16)
                if b < R:
                    rs_send[k, side, s - 1, b:R] = pairs[k, b:R, at : at + W].astype(bf16)
                rs(k, side, s).start()
            return carry

        lax.fori_loop(0, nchunk, rs_hop, 0)

    ur = lax.broadcasted_iota(jnp.int32, (RP, R), 0)
    uc = lax.broadcasted_iota(jnp.int32, (RP, R), 1)
    unpack = jnp.where((uc // cap == ur // PAD) & (uc % cap == ur % PAD), 1.0, 0.0).astype(bf16)

    def ret(d):
        p = pos[d]
        return remote(
            ret_send.at[p * PAD : (p + 1) * PAD],
            ret_recv.at[block(z)],
            ret_s.at[d],
            ret_r.at[(nz - d) % nz],
            {"ep": (z + d) % nz},
        )

    def ret_in(d):
        view = ret_recv.at[block((z + d) % nz)]
        return remote(view, view, ret_s.at[d], ret_r.at[d], {"ep": (z + d) % nz})

    for k in range(nchunk):
        for side in range(2):
            rs(k, side, half).wait_recv()
            a, b = part_rows(side, half)
            pairs[k, a:b, 0:W] = pairs[k, a:b, 0:W] + rs_recv[k, side, half - 1, a:b].astype(f32)
        y = pairs[k, :, 0:W].astype(bf16)
        ret_send[k * RP : (k + 1) * RP] = jnp.dot(unpack, y, preferred_element_type=f32).astype(
            bf16
        )
        for p in range(4 * k, 4 * k + 4):
            if p:
                ret(order[p]).start()
    ret_recv[block(z)] = ret_send[0:PAD]

    logits = logits_ref[...]
    top = jnp.max(logits, axis=-1, keepdims=True)
    ex = jnp.exp(logits - top)
    soft = ex / jnp.sum(ex, axis=-1, keepdims=True)
    eye = lax.broadcasted_iota(jnp.int32, (count, count), 0) == lax.broadcasted_iota(
        jnp.int32, (count, count), 1
    )
    gg = jnp.sum(jnp.where(eye, ggate_ref[...], 0.0), axis=1, keepdims=True)
    weights = gg * soft

    for d in order[1:]:
        ret_in(d).wait_recv()
    table = ret_recv[...]
    p0 = jnp.dot(smat[0], table, preferred_element_type=f32)
    p1 = jnp.dot(smat[1], table, preferred_element_type=f32)
    out_ref[...] = (weights[:, 0:1] * p0 + weights[:, 1:2] * p1).astype(bf16)

    for d in order[1:]:
        disp(d).wait_send()
        ret(d).wait_send()

    def drain(k, carry):
        for side in range(2):
            for s in range(1, half + 1):
                ag(k, side, s).wait_send()
                rs(k, side, s).wait_send()
        for j in range(ndd):
            dd(k, j, True).wait_send()
        pair(k).wait_send()
        return carry

    lax.fori_loop(0, nchunk, drain, 0)


def moe(mesh, rows, routes, ggate, logits, gain, wg, wu, wd):
    nz, nt = mesh.shape["ep"], mesh.shape["tp"]
    count, width = rows.shape
    nx = nt // 2
    half = nx // 2
    cap = 3 * count // nz
    k = nz // 4
    R = 4 * cap
    color = nx * W
    dma = pltpu.SemaphoreType.DMA
    vmem = pl.BlockSpec(memory_space=pltpu.VMEM)
    hbm = pl.BlockSpec(memory_space=pl.ANY)
    return pl.pallas_call(
        functools.partial(moe_kernel, nz, nt),
        out_shape=jax.ShapeDtypeStruct((count, W), bf16),
        in_specs=[hbm, vmem, vmem, vmem, vmem, hbm, hbm, hbm],
        out_specs=vmem,
        scratch_shapes=[
            pltpu.VMEM((count, width), bf16),
            pltpu.VMEM((width, 2 * W), bf16),
            pltpu.VMEM((W, width), bf16),
            pltpu.VMEM((nz * PAD, W), bf16),
            pltpu.VMEM((nz * PAD, W), bf16),
            pltpu.VMEM((k * R, width), bf16),
            pltpu.VMEM((k, R, color), f32),
            pltpu.VMEM((k, R, color), bf16),
            pltpu.VMEM((k, R, color), bf16),
            pltpu.VMEM((k, 2, half, R, W), bf16),
            pltpu.VMEM((k, 2, half, R, W), bf16),
            pltpu.VMEM((nz * PAD, W), bf16),
            pltpu.VMEM((nz * PAD, W), bf16),
            pltpu.VMEM((2, count, nz * PAD), bf16),
            dma((3,)),
            dma((2 * nx,)),
            dma((nz,)),
            dma((nz,)),
            dma((k, 2, half)),
            dma((k, 2, half)),
            dma((k, 2 * half + 1)),
            dma((k, 2 * half + 1)),
            dma((k,)),
            dma((k,)),
            dma((k, 2, half)),
            dma((k, 2, half)),
            dma((nz,)),
            dma((nz,)),
        ],
        compiler_params=pltpu.CompilerParams(collective_id=0, has_side_effects=True),
        name="moe",
    )(rows, routes, ggate, logits, gain, wg, wu, wd)


def head_norm(x, gain):
    wide = x.astype(jnp.float32)
    return wide * lax.rsqrt(jnp.mean(wide * wide, axis=-1, keepdims=True) + 1e-06) * gain


def rotate(x, first):
    count = x.shape[0]
    pos = first + jnp.arange(count, dtype=jnp.int32)
    row = (pos // GRID_W).astype(jnp.float32)
    col = (pos % GRID_W).astype(jnp.float32)
    nfreq = HEAD_DIM // 4
    inverse = 10000.0 ** (-jnp.arange(nfreq, dtype=jnp.float32) / nfreq)
    angle = jnp.concatenate(
        [
            row[:, None] * inverse,
            row[:, None] * inverse,
            col[:, None] * inverse,
            col[:, None] * inverse,
        ],
        axis=1,
    )
    parts = x.reshape(x.shape[:-1] + (2, 2, nfreq))
    turned = jnp.stack([-parts[..., 1, :], parts[..., 0, :]], axis=-2).reshape(x.shape)
    return x * jnp.cos(angle)[:, None, :] + turned * jnp.sin(angle)[:, None, :]


def attention(queries, keys, values, q_gain, k_gain, w_out):
    rows = queries.shape[0]
    heads_dev = queries.shape[1] // HEAD_DIM
    group = HEADS // KV_HEADS
    kv_dev = max(1, heads_dev // group)
    per_kv = heads_dev // kv_dev
    first_kv = lax.axis_index("tp") * heads_dev // group
    first_row = lax.axis_index("ep") * rows
    k_mine = lax.dynamic_slice_in_dim(keys, first_kv * HEAD_DIM, kv_dev * HEAD_DIM, 1)
    v_mine = lax.dynamic_slice_in_dim(values, first_kv * HEAD_DIM, kv_dev * HEAD_DIM, 1)
    k_rot = rotate(head_norm(k_mine.reshape(rows, kv_dev, HEAD_DIM), k_gain), first_row)
    k_rot = k_rot.astype(jnp.bfloat16).reshape(rows, kv_dev * HEAD_DIM)
    q_rot = rotate(head_norm(queries.reshape(rows, heads_dev, HEAD_DIM), q_gain), first_row)
    q_rot = q_rot.astype(jnp.bfloat16).reshape(rows, kv_dev, per_kv, HEAD_DIM)
    scale = HEAD_DIM ** (-0.5)
    both = lax.all_gather(jnp.concatenate([k_rot, v_mine], 1), "ep", axis=0, tiled=True)
    k_piece, v_piece = both[:, : kv_dev * HEAD_DIM], both[:, kv_dev * HEAD_DIM :]
    count = k_piece.shape[0]
    key_rows = k_piece.reshape(count, kv_dev, HEAD_DIM)
    value_rows = v_piece.reshape(count, kv_dev, HEAD_DIM)
    scores = (
        jnp.einsum("qkgd,nkd->qkgn", q_rot, key_rows, preferred_element_type=jnp.float32) * scale
    )
    top = jnp.max(scores, axis=-1)
    expo = jnp.exp(scores - top[..., None])
    total = jnp.sum(expo, axis=-1)
    acc = jnp.einsum(
        "qkgn,nkd->qkgd", expo.astype(jnp.bfloat16), value_rows, preferred_element_type=jnp.float32
    )
    mixed = (acc / total[..., None]).astype(jnp.bfloat16).reshape(rows, heads_dev * HEAD_DIM)
    return jnp.dot(
        lax.all_gather(mixed, "tp", axis=1, tiled=True), w_out, preferred_element_type=jnp.float32
    ).astype(jnp.bfloat16)


def solution(mesh):
    def per_device(
        queries, keys, values, q_gain, k_gain, w_out, moe_rows, routes,
        group_gate, expert_logits, moe_gain, w_gate, w_up, w_down,
    ):
        attn_out = attention(queries, keys, values, q_gain, k_gain, w_out)
        moe_out = moe(
            mesh,
            moe_rows,
            routes,
            group_gate.reshape(1, -1),
            expert_logits,
            moe_gain.reshape(1, -1),
            w_gate[0],
            w_up[0],
            w_down[0],
        )
        return attn_out, moe_out

    placed = (
        P(("grp", "ep"), "tp"),
        P(("grp", "ep"), None),
        P(("grp", "ep"), None),
        P(),
        P(),
        P(None, "tp"),
        P(("grp", "ep"), None),
        P(("grp", "ep"), None),
        P(("grp", "ep")),
        P(("grp", "ep"), None),
        P(),
        P("ep", None, "tp"),
        P("ep", None, "tp"),
        P("ep", "tp", None),
    )
    return jax.shard_map(
        per_device,
        mesh=mesh,
        in_specs=placed,
        out_specs=(P(("grp", "ep"), "tp"), P(("grp", "ep"), "tp")),
        check_vma=False,
    )
```

```python
import functools

import jax
import jax.numpy as jnp
from jax import lax
from jax.experimental import pallas as pl
from jax.experimental.pallas import tpu as pltpu
from jax.sharding import PartitionSpec as P

HEADS = 16
KV_HEADS = 4
HEAD_DIM = 128
GRID_W = 64
TOPK = 2
GROUP = HEADS // KV_HEADS
W = 128
PAD = 48
MESH = pl.DeviceIdType.MESH
f32 = jnp.float32
bf16 = jnp.bfloat16


def remote(src, dst, ss, rs, dev):
    return pltpu.make_async_remote_copy(
        src_ref=src, dst_ref=dst, send_sem=ss, recv_sem=rs, device_id=dev, device_id_type=MESH
    )


def near_first(n):
    order = [0]
    for i in range(1, n // 2 + 1):
        order += [i] if 2 * i == n else [i, n - i]
    return order


SCRATCH = (
    "queries_v",
    "k_raw",
    "kvb",
    "qs",
    "qgain_v",
    "kgain_v",
    "wout_v",
    "o_own",
    "lse_own",
    "po_send",
    "po_recv",
    "ls_send",
    "ls_recv",
    "heads",
    "rows_v",
    "routes_v",
    "ggate_v",
    "logits_v",
    "gain_v",
    "w13",
    "wdp",
    "sendb",
    "recvb",
    "xall",
    "pairs",
    "psend",
    "precv",
    "rs_send",
    "rs_recv",
    "ret_send",
    "ret_recv",
    "sslot",
    "smat",
    "wcol",
    "lsem",
    "wsem",
    "disp_s",
    "disp_r",
    "ag_s",
    "ag_r",
    "dd_s",
    "dd_r",
    "pr_s",
    "pr_r",
    "rss_s",
    "rss_r",
    "ret_s",
    "ret_r",
    "q_s",
    "q_r",
    "kva_s",
    "kva_r",
    "kvb_s",
    "kvb_r",
    "po_s",
    "po_r",
    "ls_s",
    "ls_r",
    "oag_s",
    "oag_r",
    "odd_s",
    "odd_r",
    "in_sem",
    "pack",
    "unpack",
)


def fused_kernel(nz, nt, *refs):
    (q_hbm, keys_hbm, values_hbm, qgain_hbm, kgain_hbm, wout_hbm, rows_hbm, routes_hbm, ggate_hbm, logits_hbm, gain_hbm, wg_hbm, wu_hbm, wd_hbm, attn_ref, out_ref) = refs[:16]
    s_ = dict(zip(SCRATCH, refs[16:], strict=True))
    queries_v, k_raw, kvb, qs, qgain_v, kgain_v, wout_v = (s_[n] for n in SCRATCH[:7])
    o_own, lse_own, po_send, po_recv, ls_send, ls_recv, heads = (s_[n] for n in SCRATCH[7:14])
    rows_v, routes_v, ggate_v, logits_v, gain_v, w13, wdp = (s_[n] for n in SCRATCH[14:21])
    sendb, recvb, xall, pairs, psend, precv, rs_send, rs_recv = (s_[n] for n in SCRATCH[21:29])
    ret_send, ret_recv, sslot, smat, wcol = (s_[n] for n in SCRATCH[29:34])
    lsem, wsem, disp_s, disp_r, ag_s, ag_r, dd_s, dd_r = (s_[n] for n in SCRATCH[34:42])
    pr_s, pr_r, rss_s, rss_r, ret_s, ret_r = (s_[n] for n in SCRATCH[42:48])
    q_s, q_r, kva_s, kva_r, kvb_s, kvb_r, po_s, po_r, ls_s, ls_r = (s_[n] for n in SCRATCH[48:58])
    oag_s, oag_r, odd_s, odd_r, in_sem, pack, unpack = (s_[n] for n in SCRATCH[58:65])

    count, width = rows_v.shape
    nx = nt // 2
    half = nx // 2
    cap = 3 * count // nz
    nchunk = nz // 4
    R = 4 * cap
    RP = 4 * PAD
    up_rows = 80
    order = near_first(nz)
    color = nx * W
    qrows = queries_v.shape[0]
    kq = qrows // GROUP
    nset = nz // 4
    setrows = nset * kq

    z = lax.axis_index("ep")
    t = lax.axis_index("tp")
    x = t // 2
    c = t % 2
    right = ((x + 1) % nx) * 2 + c
    left = ((x + nx - 1) % nx) * 2 + c
    other = x * 2 + (1 - c)
    xpair = x + 1 - 2 * (x % 2)
    mates = (None, other, xpair * 2 + c, xpair * 2 + 1 - c)
    quarter = t % GROUP
    kvh = t // GROUP

    def lane(i):
        return pl.ds(pl.multiple_of(i * W, W), W)

    with jax.named_scope("signal"):
        barrier = pltpu.get_barrier_semaphore()

        def greet(j, carry):
            @pl.when(j > z)
            def _():
                pl.semaphore_signal(barrier, inc=1, device_id={"ep": j}, device_id_type=MESH)

            return carry

        lax.fori_loop(0, nz, greet, 0)
        for who in (right, left, other, mates[2], mates[3]):
            pl.semaphore_signal(barrier, inc=1, device_id={"tp": who}, device_id_type=MESH)

        local = {}

        def fetch(name, src, dst):
            local[name] = pltpu.make_async_copy(src, dst, lsem.at[len(local)])
            local[name].start()

        fetch("routes", routes_hbm, routes_v)
        fetch("rows", rows_hbm, rows_v)
        fetch("gain", gain_hbm, gain_v)
        fetch("q", q_hbm, queries_v)
        fetch("k", keys_hbm.at[pl.ds(pl.multiple_of(quarter * kq, kq), kq), lane(kvh)], k_raw)
        fetch(
            "v",
            values_hbm.at[pl.ds(pl.multiple_of(quarter * kq, kq), kq), lane(kvh)],
            kvb.at[0:kq, W : 2 * W],
        )
        fetch("qg", qgain_hbm, qgain_v)
        fetch("kg", kgain_hbm, kgain_v)
        fetch("gg", ggate_hbm, ggate_v)
        fetch("lg", logits_hbm, logits_v)
        fetch("wg", wg_hbm, w13.at[:, 0:W])
        fetch("wu", wu_hbm, w13.at[:, W : 2 * W])
        load_d = []
        for k in range(2):
            for dx in range(nx):
                core = c if k == 0 else 1 - c
                col = ((x + dx) % nx) * 2 + core
                at = k * color + dx * W
                load_d.append(
                    pltpu.make_async_copy(
                        wd_hbm.at[:, lane(col)], wdp.at[:, at : at + W], wsem.at[k * nx + dx]
                    )
                )
                load_d[-1].start()
        fetch("wo", wout_hbm, wout_v)

    with jax.named_scope("slots"):
        local["routes"].wait()
        e_sub = lax.broadcasted_iota(jnp.int32, (nz, count), 0)
        r0 = routes_v[0:1, :]
        r1 = routes_v[1:2, :]
        named = jnp.where((r0 == e_sub) | (r1 == e_sub), 1.0, 0.0).astype(bf16)
        before = jnp.where(
            lax.broadcasted_iota(jnp.int32, (count, count), 0)
            < lax.broadcasted_iota(jnp.int32, (count, count), 1),
            1.0,
            0.0,
        ).astype(bf16)
        rank = jnp.dot(named, before, preferred_element_type=f32).astype(bf16)
        lo = lax.broadcasted_iota(jnp.int32, (nz * PAD, nz), 1) * PAD
        slot = lax.broadcasted_iota(jnp.int32, (nz * PAD, nz), 0)
        spread = jnp.where((slot >= lo) & (slot < lo + PAD), 1.0, 0.0).astype(bf16)
        slot_of = (lax.broadcasted_iota(jnp.int32, (nz * PAD, count), 0) % PAD).astype(f32)
        named_x = jnp.dot(spread, named, preferred_element_type=f32)
        rank_x = jnp.dot(spread, rank, preferred_element_type=f32)
        hit = (named_x > 0.5) & (jnp.abs(rank_x - slot_of) < 0.5)
        sslot[...] = jnp.where(hit, 1.0, 0.0)

    with jax.named_scope("norm"):
        local["rows"].wait()
        local["gain"].wait()
        wide = rows_v[...].astype(f32)
        inv = lax.rsqrt(jnp.mean(wide * wide, axis=-1, keepdims=True) + 1e-06)
        mine = rows_v[:, lane(t)].astype(f32) * inv * gain_v[:, lane(t)]
        sendb[...] = jnp.dot(
            sslot[...].astype(bf16), mine.astype(bf16), preferred_element_type=f32
        ).astype(bf16)

    with jax.named_scope("barrier"):
        pl.semaphore_wait(barrier, z + 5)

        def enter(j, carry):
            @pl.when(j < z)
            def _():
                pl.semaphore_signal(in_sem.at[z], inc=1, device_id={"ep": j}, device_id_type=MESH)

            return carry

        lax.fori_loop(0, nz, enter, 0)

    def block(i):
        return pl.ds(pl.multiple_of(i * PAD, PAD), PAD)

    def place(d):
        far = d // (nz // 2 + 1)
        return (1 - far) * (2 * d - 1) + far * 2 * (nz - d)

    def disp(j):
        p = place((z - j + nz) % nz)
        return remote(
            sendb.at[block(j)], recvb.at[block(p)], disp_s.at[j], disp_r.at[p], {"ep": j}
        )

    def disp_in(p):
        view = recvb.at[block(p)]
        return remote(view, view, disp_s.at[0], disp_r.at[p], {"ep": z})

    def turned(v, gain, first):
        n = v.shape[0]
        wide = v.astype(f32)
        v = wide * lax.rsqrt(jnp.mean(wide * wide, axis=-1, keepdims=True) + 1e-06) * gain
        p = first + lax.broadcasted_iota(jnp.int32, (n, W), 0)
        ln = lax.broadcasted_iota(jnp.int32, (n, W), 1)
        nf = HEAD_DIM // 4
        at = jnp.where(ln < 2 * nf, p // GRID_W, p % GRID_W).astype(f32)
        inverse = jnp.exp((ln % nf).astype(f32) * (-9.210340371976184 / nf))
        angle = at * inverse
        odd = (ln // nf) % 2 == 1
        h = jnp.where(odd, pltpu.roll(v, nf, 1), -pltpu.roll(v, W - nf, 1))
        return (v * jnp.cos(angle) + h * jnp.sin(angle)).astype(bf16)

    def qsend(m):
        return remote(qs.at[0], qs.at[m], q_s.at[m - 1], q_r.at[m - 1], {"tp": mates[m]})

    def kv_a(m):
        to = (z + 4 * m) % nz
        return remote(
            kvb.at[0:kq], kvb.at[pl.ds(pl.multiple_of(m * kq, kq), kq)], kva_s.at[m], kva_r.at[m], {"ep": to}
        )

    def kv_b(g):
        d = (0, 1, nz - 1, 2 + c * (nz - 4))[g]
        return remote(
            kvb.at[0:setrows],
            kvb.at[g * setrows : (g + 1) * setrows],
            kvb_s.at[g],
            kvb_r.at[g],
            {"ep": (z + d) % nz},
        )

    with jax.named_scope("rope_k"):
        local["k"].wait()
        local["kg"].wait()
        kvb[0:kq, 0:W] = turned(k_raw[...], kgain_v[...], z * qrows + quarter * kq)
        local["v"].wait()
        local["q"].wait()
        local["qg"].wait()
        qs[0] = turned(queries_v[...], qgain_v[...], z * qrows)
        for m in (2, 3, 1):
            qsend(m).start()
        recvb[0:PAD] = sendb[block(z)]
        prow = lax.broadcasted_iota(jnp.int32, (R, RP), 0)
        pcol = lax.broadcasted_iota(jnp.int32, (R, RP), 1)
        pack[...] = jnp.where(
            (prow // cap == pcol // PAD) & (prow % cap == pcol % PAD), 1.0, 0.0
        ).astype(bf16)
        urow = lax.broadcasted_iota(jnp.int32, (RP, R), 0)
        ucol = lax.broadcasted_iota(jnp.int32, (RP, R), 1)
        unpack[...] = jnp.where(
            (ucol // cap == urow // PAD) & (ucol % cap == urow % PAD), 1.0, 0.0
        ).astype(bf16)

    with jax.named_scope("dispatch"):

        def send_to(j, carry):
            @pl.when(j > z)
            def _():
                pl.semaphore_wait(in_sem.at[j], 1)

            @pl.when(j != z)
            def _():
                disp(j).start()

            d = (j - z + nz) % nz

            @pl.when((j != z) & (d % 4 == 0))
            def _():
                kv_a(d // 4).start()

            return carry

        lax.fori_loop(0, nz, send_to, 0)

    def at_rows(k):
        return pl.ds(pl.multiple_of(k * R, R), R)

    def ag(k, side, s):
        xo = (x + nx - (s - 1)) % nx if side == 0 else (x + s - 1) % nx
        cols = lane(xo * 2 + c)
        if s < half:
            part = at_rows(k)
        elif side == 0:
            part = pl.ds(pl.multiple_of(k * R, 16), up_rows)
        else:
            part = pl.ds(pl.multiple_of(k * R + up_rows, 16), R - up_rows)
        view = xall.at[part, cols]
        to = right if side == 0 else left
        return remote(view, view, ag_s.at[k, side, s - 1], ag_r.at[k, side, s - 1], {"tp": to})

    def dd_place(j):
        if j == 0:
            return x, None
        if j <= half - 1:
            return (x + nx - j) % nx, None
        if j <= 2 * half - 2:
            return (x + j - (half - 1)) % nx, None
        return (x + half) % nx, j - (2 * half - 1)

    def dd(k, j, mine_side):
        core = c if mine_side else 1 - c
        xo, far = dd_place(j)
        rows = at_rows(k)
        if far == 0:
            rows = pl.ds(pl.multiple_of(k * R, 16), up_rows)
        elif far == 1:
            rows = pl.ds(pl.multiple_of(k * R + up_rows, 16), R - up_rows)
        view = xall.at[rows, lane(xo * 2 + core)]
        return remote(view, view, dd_s.at[k, j], dd_r.at[k, j], {"tp": other})

    ndd = 2 * half + 1

    def arrive(k):
        for i in range(4):
            if i:
                disp_in(4 * k + i).wait_recv()
            else:

                @pl.when(k > 0)
                def _():
                    disp_in(4 * k).wait_recv()

        rows = pl.ds(pl.multiple_of(k * RP, RP), RP)
        packed = jnp.dot(pack[...], recvb[rows], preferred_element_type=f32)
        xall[at_rows(k), lane(t)] = packed.astype(bf16)
        ag(k, 0, 1).start()
        ag(k, 1, 1).start()
        dd(k, 0, True).start()

    def kv_second():
        with jax.named_scope("kv2"):
            for m in range(1, nset):
                kv_a(m).wait_recv()
            for g in (3, 1, 2):
                kv_b(g).start()

    def hop(k, s):
        for side in range(2):
            ag(k, side, s).wait_recv()
            if s < half:
                ag(k, side, s + 1).start()
                dd(k, s if side == 0 else half - 1 + s, True).start()
            else:
                dd(k, 2 * half - 1 + side, True).start()

    def prep():
        with jax.named_scope("prep"):
            sel = sslot[...]
            subs = lax.broadcasted_iota(jnp.int32, (nz, count), 0)
            first = jnp.where(routes_v[0:1, :] == subs, 1.0, 0.0).astype(bf16)
            low = lax.broadcasted_iota(jnp.int32, (nz * PAD, nz), 1) * PAD
            at = lax.broadcasted_iota(jnp.int32, (nz * PAD, nz), 0)
            expand = jnp.where((at >= low) & (at < low + PAD), 1.0, 0.0).astype(bf16)
            s_0 = jnp.where(jnp.dot(expand, first, preferred_element_type=f32) > 0.5, sel, 0.0)
            smat[0] = s_0.T.astype(bf16)
            smat[1] = (sel - s_0).T.astype(bf16)
            local["lg"].wait()
            local["gg"].wait()
            logits = logits_v[...]
            top = jnp.max(logits, axis=0, keepdims=True)
            ex = jnp.exp(logits - top)
            weights = ggate_v[...] * (ex / jnp.sum(ex, axis=0, keepdims=True))
            eye = lax.broadcasted_iota(jnp.int32, (count, count), 0) == lax.broadcasted_iota(
                jnp.int32, (count, count), 1
            )
            for e in range(2):
                col = jnp.sum(jnp.where(eye, weights[e : e + 1, :], 0.0), axis=1, keepdims=True)
                wcol[e] = jnp.broadcast_to(col, (count, W))
            local["wg"].wait()
            local["wu"].wait()
            local["wo"].wait()
            for cp in load_d:
                cp.wait()

    def pair(k):
        return remote(psend.at[k], precv.at[k], pr_s.at[k], pr_r.at[k], {"tp": other})

    def ffn(k):
        for j in range(ndd):
            dd(k, j, False).wait_recv()
        xk = xall[at_rows(k), :]
        h = jnp.dot(xk, w13[...], preferred_element_type=f32)
        g = h[:, 0:W]
        hidden = (g * jax.nn.sigmoid(g) * h[:, W : 2 * W]).astype(bf16)
        part = jnp.dot(hidden, wdp[...], preferred_element_type=f32).astype(bf16)
        psend[k] = part[:, color:]
        pairs[k] = part[:, :color].astype(f32)
        pair(k).start()

    def part_rows(side, s):
        if s > 1:
            return 0, R
        return (0, up_rows) if side == 0 else (up_rows, R)

    def rs(k, side, s):
        a, b = part_rows(side, s)
        to = right if side == 0 else left
        return remote(
            rs_send.at[k, side, s - 1, a:b],
            rs_recv.at[k, side, s - 1, a:b],
            rss_s.at[k, side, s - 1],
            rss_r.at[k, side, s - 1],
            {"tp": to},
        )

    def target(side, s):
        far = half + 1 - s
        return far if side == 0 else nx - far

    def rs_first(k):
        pair(k).wait_recv()
        pairs[k] = pairs[k] + precv[k].astype(f32)
        for side in range(2):
            a, b = part_rows(side, 1)
            at = target(side, 1) * W
            rs_send[k, side, 0, a:b] = pairs[k, a:b, at : at + W].astype(bf16)
            rs(k, side, 1).start()

    def rs_hop(k, s):
        for side in range(2):
            rs(k, side, s - 1).wait_recv()
            at = target(side, s) * W
            a, b = part_rows(side, s - 1)
            rs_send[k, side, s - 1, a:b] = (
                pairs[k, a:b, at : at + W] + rs_recv[k, side, s - 2, a:b].astype(f32)
            ).astype(bf16)
            if a > 0:
                rs_send[k, side, s - 1, 0:a] = pairs[k, 0:a, at : at + W].astype(bf16)
            if b < R:
                rs_send[k, side, s - 1, b:R] = pairs[k, b:R, at : at + W].astype(bf16)
            rs(k, side, s).start()

    def po(m):
        return remote(
            po_send.at[m - 1], po_recv.at[m - 1], po_s.at[m - 1], po_r.at[m - 1], {"tp": mates[m]}
        )

    def ls(m):
        return remote(
            ls_send.at[m - 1], ls_recv.at[m - 1], ls_s.at[m - 1], ls_r.at[m - 1], {"tp": mates[m]}
        )

    def attend(q):
        sc = lax.dot_general(
            q, kvb[:, 0:W], (((1,), (1,)), ((), ())), preferred_element_type=f32
        ) * (HEAD_DIM**-0.5)
        top = jnp.max(sc, axis=-1, keepdims=True)
        ex = jnp.exp(sc - top)
        total = jnp.sum(ex, axis=-1, keepdims=True)
        o = jnp.dot(ex.astype(bf16), kvb[:, W : 2 * W], preferred_element_type=f32) / total
        return o, jnp.broadcast_to(top + jnp.log(total), (qrows, W))

    def attend_all():
        with jax.named_scope("attwait"):
            for g in range(1, 4):
                kv_b(g).wait_recv()
            for m in (1, 2, 3):
                qsend(m).wait_recv()
        with jax.named_scope("attend"):
            for m in (2, 3, 1, 0):
                o, lse = attend(qs[m])
                if m:
                    po_send[m - 1] = o.astype(bf16)
                    ls_send[m - 1] = lse.T[0:8]
                    po(m).start()
                    ls(m).start()
                else:
                    o_own[...] = o
                    lse_own[...] = lse

    def oag(side, s):
        xo = (x + nx - (s - 1)) % nx if side == 0 else (x + s - 1) % nx
        hr = qrows // 2
        part = pl.ds(0, qrows) if s < half else pl.ds(side * hr, hr)
        view = heads.at[part, lane(xo * 2 + c)]
        to = right if side == 0 else left
        return remote(view, view, oag_s.at[side, s - 1], oag_r.at[side, s - 1], {"tp": to})

    def odd(j, mine_side):
        core = c if mine_side else 1 - c
        xo, far = dd_place(j)
        hr = qrows // 2
        part = pl.ds(0, qrows) if far is None else pl.ds(far * hr, hr)
        view = heads.at[part, lane(xo * 2 + core)]
        return remote(view, view, odd_s.at[j], odd_r.at[j], {"tp": other})

    def merge():
        with jax.named_scope("merge"):
            for m in (1, 2, 3):
                ls(m).wait_recv()
                po(m).wait_recv()
            parts = [lse_own[...]] + [
                jnp.broadcast_to(ls_recv[m, 0:1, :], (W, qrows)).T for m in range(3)
            ]
            top = jnp.maximum(jnp.maximum(parts[0], parts[1]), jnp.maximum(parts[2], parts[3]))
            den = jnp.exp(parts[0] - top)
            num = den * o_own[...]
            for m in range(3):
                wt = jnp.exp(parts[m + 1] - top)
                den = den + wt
                num = num + wt * po_recv[m].astype(f32)
            heads[:, lane(t)] = (num / den).astype(bf16)
            oag(0, 1).start()
            oag(1, 1).start()
            odd(0, True).start()

    def oag_hop(s):
        with jax.named_scope(f"oag{s}"):
            for side in range(2):
                oag(side, s).wait_recv()
                if s < half:
                    oag(side, s + 1).start()
                    odd(s if side == 0 else half - 1 + s, True).start()
                else:
                    odd(2 * half - 1 + side, True).start()

    def ret(d, p):
        return remote(
            ret_send.at[block(p)],
            ret_recv.at[block(z)],
            ret_s.at[d],
            ret_r.at[(nz - d) % nz],
            {"ep": (z + d) % nz},
        )

    def ret_in(d):
        view = ret_recv.at[block((z + d) % nz)]
        return remote(view, view, ret_s.at[d], ret_r.at[d], {"ep": (z + d) % nz})

    def back(k):
        for side in range(2):
            rs(k, side, half).wait_recv()
            a, b = part_rows(side, half)
            pairs[k, a:b, 0:W] = pairs[k, a:b, 0:W] + rs_recv[k, side, half - 1, a:b].astype(f32)
        y = pairs[k, :, 0:W].astype(bf16)
        rows = pl.ds(pl.multiple_of(k * RP, RP), RP)
        ret_send[rows] = jnp.dot(unpack[...], y, preferred_element_type=f32).astype(bf16)
        for i in range(4):
            d = 2 * k + (i + 1) // 2 if i % 2 else (nz - 2 * k - i // 2) % nz
            if i:
                ret(d, 4 * k + i).start()
            else:

                @pl.when(k > 0)
                def _(d=d):
                    ret(d, 4 * k).start()

    stages = [("arrive", arrive)]
    stages += [(f"hop{s}", functools.partial(hop, s=s)) for s in range(1, half + 1)]
    stages += [("ffn", ffn), ("rs1", rs_first)]
    stages += [(f"rs{s}", functools.partial(rs_hop, s=s)) for s in range(2, half + 1)]
    stages += [("back", back)]
    steps = nchunk + len(stages) - 1
    events = [(1, prep), (3, kv_second), (6, attend_all), (8, merge)]
    events += [(8 + s, functools.partial(oag_hop, s)) for s in range(1, half + 1)]

    def wave(step, carry):
        for n in range(len(stages) - 1, -1, -1):
            name, run = stages[n]

            @pl.when((step >= n) & (step < n + nchunk))
            def _(n=n, name=name, run=run):
                with jax.named_scope(name):
                    run(step - n)

        for at, run in events:
            pl.when(step == min(at, steps - 1))(run)
        return carry

    lax.fori_loop(0, steps, wave, 0)
    ret_recv[block(z)] = ret_send[0:PAD]

    with jax.named_scope("project"):
        for j in range(ndd):
            odd(j, False).wait_recv()
        attn_ref[...] = jnp.dot(heads[...], wout_v[...], preferred_element_type=f32).astype(bf16)

    with jax.named_scope("retwait"):
        for d in order[1:]:
            ret_in(d).wait_recv()
    with jax.named_scope("combine"):
        table = ret_recv[...]
        p0 = jnp.dot(smat[0], table, preferred_element_type=f32)
        p1 = jnp.dot(smat[1], table, preferred_element_type=f32)
        out_ref[...] = (wcol[0] * p0 + wcol[1] * p1).astype(bf16)

    with jax.named_scope("drain"):

        def sent(j, carry):
            @pl.when(j != z)
            def _():
                disp(j).wait_send()

            return carry

        lax.fori_loop(0, nz, sent, 0)
        for d in range(1, nz):
            ret(d, 0).wait_send()
        for m in range(1, nset):
            kv_a(m).wait_send()
        for m in (1, 2, 3):
            kv_b(m).wait_send()
            qsend(m).wait_send()
            po(m).wait_send()
            ls(m).wait_send()
        for j in range(ndd):
            odd(j, True).wait_send()
        for side in range(2):
            for s in range(1, half + 1):
                oag(side, s).wait_send()

        def drain(k, carry):
            for side in range(2):
                for s in range(1, half + 1):
                    ag(k, side, s).wait_send()
                    rs(k, side, s).wait_send()
            for j in range(ndd):
                dd(k, j, True).wait_send()
            pair(k).wait_send()
            return carry

        lax.fori_loop(0, nchunk, drain, 0)


def fused(mesh, queries, keys, values, qg, kg, wo, rows, routes, gg, lg, gain, wgate, wup, wdown):
    nz, nt = mesh.shape["ep"], mesh.shape["tp"]
    count, width = rows.shape
    qrows = queries.shape[0]
    kq = qrows // GROUP
    nx = nt // 2
    half = nx // 2
    cap = 3 * count // nz
    k = nz // 4
    R = 4 * cap
    color = nx * W
    ndd = 2 * half + 1
    dma = pltpu.SemaphoreType.DMA
    V = pltpu.VMEM
    shapes = dict(
        queries_v=V((qrows, W), bf16),
        k_raw=V((kq, W), bf16),
        kvb=V((nz * kq, 2 * W), bf16),
        qs=V((GROUP, qrows, W), bf16),
        qgain_v=V((1, W), f32),
        kgain_v=V((1, W), f32),
        wout_v=V((nt * W, W), bf16),
        o_own=V((qrows, W), f32),
        lse_own=V((qrows, W), f32),
        po_send=V((3, qrows, W), bf16),
        po_recv=V((3, qrows, W), bf16),
        ls_send=V((3, 8, qrows), f32),
        ls_recv=V((3, 8, qrows), f32),
        heads=V((qrows, nt * W), bf16),
        rows_v=V((count, width), bf16),
        routes_v=V((2, count), jnp.int32),
        ggate_v=V((1, count), f32),
        logits_v=V((2, count), f32),
        gain_v=V((1, width), f32),
        w13=V((width, 2 * W), bf16),
        wdp=V((W, width), bf16),
        sendb=V((nz * PAD, W), bf16),
        recvb=V((nz * PAD, W), bf16),
        xall=V((k * R, width), bf16),
        pairs=V((k, R, color), f32),
        psend=V((k, R, color), bf16),
        precv=V((k, R, color), bf16),
        rs_send=V((k, 2, half, R, W), bf16),
        rs_recv=V((k, 2, half, R, W), bf16),
        ret_send=V((nz * PAD, W), bf16),
        ret_recv=V((nz * PAD, W), bf16),
        sslot=V((nz * PAD, count), f32),
        smat=V((2, count, nz * PAD), bf16),
        wcol=V((2, count, W), f32),
        lsem=dma((16,)),
        wsem=dma((2 * nx,)),
        disp_s=dma((nz,)),
        disp_r=dma((nz,)),
        ag_s=dma((k, 2, half)),
        ag_r=dma((k, 2, half)),
        dd_s=dma((k, ndd)),
        dd_r=dma((k, ndd)),
        pr_s=dma((k,)),
        pr_r=dma((k,)),
        rss_s=dma((k, 2, half)),
        rss_r=dma((k, 2, half)),
        ret_s=dma((nz,)),
        ret_r=dma((nz,)),
        q_s=dma((3,)),
        q_r=dma((3,)),
        kva_s=dma((k,)),
        kva_r=dma((k,)),
        kvb_s=dma((4,)),
        kvb_r=dma((4,)),
        po_s=dma((3,)),
        po_r=dma((3,)),
        ls_s=dma((3,)),
        ls_r=dma((3,)),
        oag_s=dma((2, half)),
        oag_r=dma((2, half)),
        odd_s=dma((ndd,)),
        odd_r=dma((ndd,)),
        in_sem=pltpu.SemaphoreType.REGULAR((nz,)),
        pack=V((R, 4 * PAD), bf16),
        unpack=V((4 * PAD, R), bf16),
    )
    vmem = pl.BlockSpec(memory_space=pltpu.VMEM)
    hbm = pl.BlockSpec(memory_space=pl.ANY)
    return pl.pallas_call(
        functools.partial(fused_kernel, nz, nt),
        out_shape=(
            jax.ShapeDtypeStruct((qrows, W), bf16),
            jax.ShapeDtypeStruct((count, W), bf16),
        ),
        in_specs=[hbm] * 14,
        out_specs=(vmem, vmem),
        scratch_shapes=[shapes[n] for n in SCRATCH],
        compiler_params=pltpu.CompilerParams(collective_id=0, has_side_effects=True),
        name="fused",
    )(
        queries,
        keys,
        values,
        qg.reshape(1, -1),
        kg.reshape(1, -1),
        wo,
        rows,
        routes.T,
        gg.reshape(1, -1),
        lg.T,
        gain.reshape(1, -1),
        wgate[0],
        wup[0],
        wdown[0],
    )


def solution(mesh):
    placed = (
        P(("grp", "ep"), "tp"),
        P(("grp", "ep"), None),
        P(("grp", "ep"), None),
        P(),
        P(),
        P(None, "tp"),
        P(("grp", "ep"), None),
        P(("grp", "ep"), None),
        P(("grp", "ep")),
        P(("grp", "ep"), None),
        P(),
        P("ep", None, "tp"),
        P("ep", None, "tp"),
        P("ep", "tp", None),
    )
    return jax.shard_map(
        functools.partial(fused, mesh),
        mesh=mesh,
        in_specs=placed,
        out_specs=(P(("grp", "ep"), "tp"), P(("grp", "ep"), "tp")),
        check_vma=False,
    )
```
